32 devices in a mesh: sp: 8 (over z, y), tp: 4 (over x, core).
Axes of the slice: x: 2, y: 2, z: 4, core: 2. Of those that a mesh axis runs over, the one named last changes fastest.
Arguments:
- resid: bfloat16 [8192, 2048], P(('sp', 'tp')), may hold values from -6 to 6
- queries: bfloat16 [8192, 2048], P('sp', 'tp'), may hold values from -6 to 6
- keys: bfloat16 [8192, 2048], P('sp', 'tp'), may hold values from -6 to 6
- values: bfloat16 [8192, 4096], P('sp', 'tp'), may hold values from -6 to 6
- gates: bfloat16 [8192, 4096], P('sp', 'tp'), may hold values from -6 to 6
- log_decay: float32 [8, 8192], P('tp', 'sp'), may hold values from -1 to 0
- retention_output_weight: bfloat16 [4096, 2048], P('tp'), may hold values from -0.125 to 0.125
- norm_gain: bfloat16 [2048], replicated, may hold values from 0.099609375 to 1.8984375
- up_weight: bfloat16 [2048, 8192], P('sp', 'tp'), may hold values from -0.125 to 0.125
- down_weight: bfloat16 [8192, 2048], P('tp', 'sp'), may hold values from -0.0625 to 0.0625
Outputs:
- layer_out: bfloat16 [8192, 2048], P(('sp', 'tp'))
The draws below stay inside these ranges and needn't reach their ends.
All inputs are finite; a program needn't handle non-finite values.
Results may differ from the reference program's by a relative error of at most 0.02.
Values may be sent and summed in bfloat16 or wider, within the bound.
No kernel may reach another device: no remote copies, remote signals or barrier semaphores. Data moves between devices by JAX's collectives and lax.ppermute only.
A program may use at most 128 MiB of HBM per device.

```python
import math
import jax
import jax.numpy as jnp
from jax import lax

D = 2048
HEADS = 8
DK = 256
DV = 512
FF = 8192
BLOCK = 128
TOK_DEV = 1024
SEQ = 8192
N_TP = 4


def draw_log_decay(key, part):
    key_sequence_order, key_reach, key_block, key_jitter, key_place, key_keep = jax.random.split(jax.random.fold_in(key, 7), 6)
    order = jax.random.permutation(key_sequence_order, HEADS)
    fast = order < HEADS // 2
    reach = jnp.exp(jax.random.uniform(key_reach, (HEADS,), jnp.float32, math.log(30.0), math.log(100.0)))
    fast_rate = -math.log(10.0) / reach
    slow_rate = jnp.full((HEADS,), -0.1 * math.log(10.0) / SEQ, jnp.float32)
    rate = jnp.where(fast, fast_rate, slow_rate)
    segments = SEQ // TOK_DEV
    factor = jnp.exp(jax.random.uniform(key_block, (HEADS, segments, 1), jnp.float32, math.log(0.5), math.log(2.0)))
    jitter = jnp.exp(jax.random.uniform(key_jitter, (HEADS, segments, TOK_DEV), jnp.float32, -0.5, 0.5))
    per_token_slot = (rate[:, None, None] * factor * jitter).reshape(HEADS, SEQ)
    places = jax.random.randint(key_place, (HEADS, 2), 0, SEQ)
    surviving_items = jax.random.uniform(key_keep, (HEADS, 2), jnp.float32, 0.5, 0.8)
    agreement_count = jnp.arange(SEQ)[None, None, :] == places[:, :, None]
    cluster_bundles = jnp.sum(jnp.where(agreement_count, jnp.log(surviving_items)[:, :, None], 0.0), axis=1)
    return (per_token_slot + cluster_bundles).astype(jnp.float32)


def block_scale(key, dims, cuts, smallest, top_value):
    loudness, own = 1.0, jax.random.fold_in(key, 6)
    for dim, blocks in cuts:
        draws = jnp.exp(jax.random.uniform(jax.random.fold_in(own, dim), (blocks,), jnp.float32, smallest / len(cuts), top_value / len(cuts)))
        loudness = loudness * jnp.repeat(draws, dims[dim] // blocks).reshape([-1 if axis == dim else 1 for axis in range(len(dims))])
    return loudness


def normal_values(rng, dims, scale, limit, pieces=(), held_as=jnp.bfloat16):
    array = scale * jax.random.normal(rng, dims, jnp.float32)
    if pieces:
        array = array * block_scale(rng, dims, pieces, -0.22, 0.18)
    return jnp.clip(array, -limit, limit).astype(held_as)


def setup_inputs(seed: int = 0) -> dict:
    arg_keys = jax.random.split(jax.random.key(seed), 11)
    return {
        "resid": normal_values(arg_keys[0], (SEQ, D), 1.0, 6.0, ((0, 32),)),
        "queries": normal_values(arg_keys[1], (SEQ, HEADS * DK), 1.0, 6.0, ((0, 8), (1, 4))),
        "keys": normal_values(arg_keys[2], (SEQ, HEADS * DK), 1.0, 6.0, ((0, 8), (1, 4))),
        "values": normal_values(arg_keys[3], (SEQ, HEADS * DV), 1.0, 6.0, ((0, 8), (1, 4))),
        "gates": normal_values(arg_keys[4], (SEQ, HEADS * DV), 1.0, 6.0, ((0, 8), (1, 4))),
        "log_decay": draw_log_decay(jax.random.fold_in(arg_keys[10], 71), 0),
        "retention_output_weight": normal_values(arg_keys[6], (HEADS * DV, D), (HEADS * DV // 2) ** -0.5, 0.125, ((0, 4),)),
        "norm_gain": jnp.clip(1.0 + 0.18 * jax.random.normal(arg_keys[7], (D,), jnp.float32), 0.099609375, 1.8984375).astype(jnp.bfloat16),
        "up_weight": normal_values(arg_keys[8], (D, FF), D ** -0.5, 0.125, ((0, 8), (1, 4))),
        "down_weight": normal_values(arg_keys[9], (FF, D), FF ** -0.5, 0.0625, ((0, 4), (1, 8))),
    }


tiny_stabilizer = 1e-06

def round_trip(values_in):
    return lax.optimization_barrier(values_in.astype(jnp.bfloat16)).astype(jnp.float32)

def rotate(values_in, token_indices):
    half_width = values_in.shape[-1] // 2
    inverse = 10000.0 ** (-jnp.arange(0, 2 * half_width, 2, dtype=jnp.float32) / (2 * half_width))
    angles = token_indices[:, None].astype(jnp.float32) * inverse[None, :]
    cosine = jnp.cos(angles)[:, None, :]
    sine_lookup = jnp.sin(angles)[:, None, :]
    first_half = values_in[..., :half_width]
    second = values_in[..., half_width:]
    return jnp.concatenate([first_half * cosine - second * sine_lookup, first_half * sine_lookup + second * cosine], axis=-1)

def normalize(updated, norm_gain):
    widened = updated.astype(jnp.float32)
    scaled = widened * lax.rsqrt(lax.optimization_barrier(jnp.mean(widened * widened, axis=-1, keepdims=True)) + tiny_stabilizer)
    return (scaled * norm_gain.astype(jnp.float32)).astype(jnp.bfloat16)

def block_step(carry_state, per_block):
    query_blk, key_blk, value_blk, gate_blk, cum_blk = per_block
    length = cum_blk.shape[1]
    causal = jnp.arange(length)[:, None] >= jnp.arange(length)[None, :]
    spread = cum_blk[:, :, None] - cum_blk[:, None, :]
    factor = jnp.where(causal[None], jnp.exp(jnp.minimum(spread, 0.0)), 0.0)
    scores = jnp.einsum('ihd,jhd->hij', query_blk, key_blk)
    weights = round_trip(scores * factor)
    within_block = jnp.einsum('hij,jhv->ihv', weights, value_blk)
    decayed = round_trip(query_blk * jnp.exp(cum_blk).T[:, :, None])
    carried_part = jnp.einsum('ihd,hdv->ihv', decayed, round_trip(carry_state))
    retained = within_block + carried_part
    normed = retained * lax.rsqrt(lax.optimization_barrier(jnp.mean(retained * retained, axis=-1, keepdims=True)) + tiny_stabilizer)
    gated_out = (jax.nn.silu(gate_blk) * normed).astype(jnp.bfloat16)
    tile_count_all = cum_blk[:, -1]
    key_decayed = round_trip(key_blk * jnp.exp(tile_count_all[:, None] - cum_blk).T[:, :, None])
    update = jnp.einsum('jhd,jhv->hdv', key_decayed, value_blk)
    return (jnp.exp(tile_count_all)[:, None, None] * carry_state + update, gated_out)

def grouped_product(left, right, groups):
    group_width = left.shape[1] // groups

    def add_group(running, number):
        first_row = (number * group_width).astype(jnp.int32)
        left_part = lax.dynamic_slice_in_dim(left, first_row, group_width, 1)
        right_part = lax.dynamic_slice_in_dim(right, first_row, group_width, 0)
        partial_value = jnp.dot(left_part, right_part, preferred_element_type=jnp.float32)
        return (running + round_trip(partial_value), None)
    running = jnp.zeros((left.shape[0], right.shape[1]), jnp.float32)
    running, unused = lax.scan(add_group, running, jnp.arange(groups, dtype=jnp.int32))
    return running

def channel_mixer(normed, up_weight, down_weight, groups):
    group_width = up_weight.shape[1] // groups

    def add_group(running, number):
        first_row = (number * group_width).astype(jnp.int32)
        up_part = lax.dynamic_slice_in_dim(up_weight, first_row, group_width, 1)
        down_part = lax.dynamic_slice_in_dim(down_weight, first_row, group_width, 0)
        preact = jnp.maximum(jnp.dot(normed, up_part, preferred_element_type=jnp.float32), 0.0)
        hidden = (preact * preact).astype(jnp.bfloat16)
        partial_value = jnp.dot(hidden, down_part, preferred_element_type=jnp.float32)
        return (running + round_trip(partial_value), None)
    running = jnp.zeros((normed.shape[0], down_weight.shape[1]), jnp.float32)
    running, unused = lax.scan(add_group, running, jnp.arange(groups, dtype=jnp.int32))
    return running

def reference(resid, queries, keys, values, gates, log_decay, retention_output_weight, norm_gain, up_weight, down_weight):
    length = queries.shape[0]
    blocks = length // BLOCK
    token_indices = jnp.arange(length, dtype=jnp.int32)
    query_rot = round_trip(rotate(queries.astype(jnp.float32).reshape(length, HEADS, DK), token_indices))
    key_rot = round_trip(rotate(keys.astype(jnp.float32).reshape(length, HEADS, DK), token_indices) * DK ** (-0.5))
    cumulative = jnp.cumsum(log_decay.astype(jnp.float32).reshape(HEADS, blocks, BLOCK), axis=2)
    per_block = (query_rot.reshape(blocks, BLOCK, HEADS, DK), key_rot.reshape(blocks, BLOCK, HEADS, DK), values.astype(jnp.float32).reshape(blocks, BLOCK, HEADS, DV), gates.astype(jnp.float32).reshape(blocks, BLOCK, HEADS, DV), jnp.moveaxis(cumulative, 1, 0))
    unused, gated_out = lax.scan(block_step, jnp.zeros((HEADS, DK, DV), jnp.float32), per_block)
    gated_out = gated_out.reshape(length, HEADS * DV)
    mixed_sum = grouped_product(gated_out, retention_output_weight, N_TP)
    updated = (resid.astype(jnp.float32) + mixed_sum).astype(jnp.bfloat16)
    normed = normalize(updated, norm_gain)
    channel_sum = channel_mixer(normed, up_weight, down_weight, N_TP)
    return (updated.astype(jnp.float32) + channel_sum).astype(jnp.bfloat16)
```

```python
import functools

import jax
import jax.numpy as jnp
from jax import lax
from jax.experimental import pallas as pl
from jax.experimental.pallas import tpu as pltpu
from jax.sharding import PartitionSpec as P


DK = 256
DV = 512
BLOCK = 128
EPS = 1e-06
BF = jnp.bfloat16
F32 = jnp.float32
TAIL = 16


def params(mib=48):
    return pltpu.CompilerParams(vmem_limit_bytes=mib * 1024 * 1024)


def dot(a, b, contract=((1,), (0,))):
    return lax.dot_general(a, b, (contract, ((), ())), preferred_element_type=F32)


def decay_sums(log_decay):
    blocks = log_decay.shape[0]
    lane = lax.broadcasted_iota(jnp.int32, (blocks, BLOCK), 1)
    row = lax.broadcasted_iota(jnp.int32, (blocks, BLOCK), 0)
    cum = log_decay
    step = 1
    while step < BLOCK:
        cum = cum + jnp.where(lane >= step, pltpu.roll(cum, step, 1), 0.0)
        step *= 2
    total = jnp.broadcast_to(cum[:, BLOCK - 1 :], (blocks, BLOCK))
    upto = total
    step = 1
    while step < blocks:
        upto = upto + jnp.where(row >= step, pltpu.roll(upto, step, 0), 0.0)
        step *= 2
    padded = jnp.concatenate([cum, jnp.zeros((BLOCK - blocks, BLOCK), F32)], axis=0)
    return cum, padded.T, total, upto - total, upto[blocks - 1 :, :]


def turned(part, n, table_ref):
    half = part.shape[1] // 2
    cos_r, sin_r = table_ref[0, :BLOCK, :], table_ref[1, :BLOCK, :]
    cos_b, sin_b = table_ref[0, BLOCK + n : BLOCK + n + 1, :], table_ref[1, BLOCK + n : BLOCK + n + 1, :]
    cosine = cos_r * cos_b - sin_r * sin_b
    sine = sin_r * cos_b + cos_r * sin_b
    first, second = part[:, :half].astype(F32), part[:, half:].astype(F32)
    return first * cosine - second * sine, first * sine + second * cosine


def state_kernel(key_ref, value_ref, decay_ref, table_ref, out_ref, kd_ref, *, halves):
    blocks = decay_ref.shape[1]
    _, col, _, before, whole = decay_sums(decay_ref[0])
    scale = DK ** (-0.5)
    for n in range(blocks):
        rows = pl.ds(n * BLOCK, BLOCK)
        a, b = turned(key_ref[rows, :], n, table_ref)
        a, b = (a * scale).astype(BF).astype(F32), (b * scale).astype(BF).astype(F32)
        factor = jnp.exp(whole - before[n : n + 1, :] - jnp.broadcast_to(col[:, n : n + 1], (BLOCK, BLOCK)))
        kd_ref[rows, : DK // 2] = (a * factor).astype(BF)
        kd_ref[rows, DK // 2 :] = (b * factor).astype(BF)
    state = dot(kd_ref[...], value_ref[...], ((0,), (0,))).astype(BF)
    decay = jnp.broadcast_to(jnp.exp(whole[:, :1]), (TAIL, DV))
    high = decay.astype(BF).astype(F32)
    row = lax.broadcasted_iota(jnp.int32, (TAIL, DV), 0)
    tail = jnp.where(row == 0, high, decay - high).astype(BF)
    size = DK // halves
    for j in range(halves):
        out_ref[j, :size, :] = state[j * size : (j + 1) * size, :]
        out_ref[j, size:, :] = tail


def local_kernel(query_ref, key_ref, value_ref, decay_ref, table_ref, out_ref, qd_ref, state_ref):
    blocks = decay_ref.shape[1]
    cum, col, total, before, _ = decay_sums(decay_ref[0])
    scale = DK ** (-0.5)
    causal = lax.broadcasted_iota(jnp.int32, (BLOCK, BLOCK), 0) >= lax.broadcasted_iota(
        jnp.int32, (BLOCK, BLOCK), 1
    )
    for n in range(blocks):
        rows = pl.ds(n * BLOCK, BLOCK)
        qa, qb = turned(query_ref[rows, :], n, table_ref)
        ka, kb = turned(key_ref[rows, :], n, table_ref)
        qa, qb = qa.astype(BF), qb.astype(BF)
        ka, kb = (ka * scale).astype(BF), (kb * scale).astype(BF)
        query = jnp.concatenate([qa, qb], axis=1)
        key = jnp.concatenate([ka, kb], axis=1)
        value = value_ref[rows, :]
        down = jnp.broadcast_to(col[:, n : n + 1], (BLOCK, BLOCK))
        spread = down - cum[n : n + 1, :]
        factor = jnp.where(causal, jnp.exp(jnp.minimum(spread, 0.0)), 0.0)
        weights = (dot(query, key, ((1,), (1,))) * factor).astype(BF)
        result = dot(weights, value)
        from_block = jnp.exp(down)
        if n:
            near = jnp.concatenate(
                [(qa.astype(F32) * from_block).astype(BF), (qb.astype(F32) * from_block).astype(BF)], axis=1
            )
            result = result + dot(near, state_ref[...].astype(BF))
        out_ref[rows, :] = result
        from_start = jnp.exp(down + before[n : n + 1, :])
        qd_ref[rows, : DK // 2] = (qa.astype(F32) * from_start).astype(BF)
        qd_ref[rows, DK // 2 :] = (qb.astype(F32) * from_start).astype(BF)
        if n + 1 < blocks:
            to_end = jnp.exp(total[n : n + 1, :] - down)
            kd = jnp.concatenate(
                [(ka.astype(F32) * to_end).astype(BF), (kb.astype(F32) * to_end).astype(BF)], axis=1
            )
            term = dot(kd, value, ((0,), (0,)))
            if n:
                state_ref[...] = jnp.exp(total[n : n + 1, :1]) * state_ref[...] + term
            else:
                state_ref[...] = term


def gate_kernel(order_ref, local_ref, qd_ref, in_ref, gate_ref, weight_ref, out_ref, gated_ref):
    heads = local_ref.shape[1] // DV
    for h in range(heads):
        cols = pl.ds(h * DV, DV)
        retained = local_ref[:, cols] + dot(qd_ref[:, pl.ds(h * DK, DK)], in_ref[h])
        mean = jnp.mean(retained * retained, axis=-1, keepdims=True)
        gate = gate_ref[:, cols].astype(F32)
        silu = gate / (1.0 + jnp.exp(-gate))
        gated_ref[:, cols] = (silu * (retained * lax.rsqrt(mean + EPS))).astype(BF)
    out_ref[0] = dot(gated_ref[...], weight_ref[...]).astype(BF)


def norm_kernel(y_ref, resid_ref, a_ref, b_ref, *rest, regions):
    far, (gain_ref, updated_ref, normed_ref) = rest[:-3], rest[-3:]
    mixed = a_ref[...].astype(F32) + b_ref[...].astype(F32)
    for ref in far:
        mixed = mixed + ref[...].astype(F32)
    updated = (resid_ref[...].astype(F32) + mixed).astype(BF)
    updated_ref[...] = updated
    wide = updated.astype(F32)
    scaled = wide * lax.rsqrt(jnp.mean(wide * wide, axis=-1, keepdims=True) + EPS)
    normed = (scaled * gain_ref[...].astype(F32)).astype(BF)
    size = normed.shape[1] // regions
    half = regions // 2
    lower = y_ref[0] == 0
    for r in range(half):
        even = normed[:, 2 * r * size : (2 * r + 1) * size]
        odd = normed[:, (2 * r + 1) * size : (2 * r + 2) * size]
        normed_ref[:, r * size : (r + 1) * size] = jnp.where(lower, even, odd)
        normed_ref[:, (half + r) * size : (half + r + 1) * size] = jnp.where(lower, odd, even)


def last_kernel(y_ref, updated_ref, *rest, regions):
    left_ref, right_ref, out_ref = rest
    size = 2 * left_ref.shape[1] // regions
    half = regions // 2
    lower = y_ref[0] == 0
    for r in range(half):
        own = left_ref[:, r * size : (r + 1) * size]
        other = right_ref[:, r * size : (r + 1) * size]
        even, odd = pl.ds(2 * r * size, size), pl.ds((2 * r + 1) * size, size)
        out_ref[:, even] = (updated_ref[:, even].astype(F32) + jnp.where(lower, own, other)).astype(BF)
        out_ref[:, odd] = (updated_ref[:, odd].astype(F32) + jnp.where(lower, other, own)).astype(BF)


def region_offsets(z_ref, planes, size, sides):
    offsets = []
    for side in range(sides):
        for s in range(planes):
            plane = lax.rem(z_ref[0] + (planes - s), planes)
            offsets.append(pl.multiple_of((side * planes + plane) * size, size))
    return offsets


def up_kernel(z_ref, *rest, planes, sources):
    rows, up, hidden_ref = rest[:sources], rest[sources:-1], rest[-1]
    size, units = up[0].shape
    offsets = region_offsets(z_ref, planes, size, 2)
    chunk = min(256, units)
    start = 0
    for ref in rows:
        place = pl.ds(start, ref.shape[0])
        start += ref.shape[0]
        for c in range(units // chunk):
            cols = pl.ds(c * chunk, chunk)
            acc = dot(ref[:, pl.ds(offsets[0], size)], up[0][:, cols])
            for j in range(1, len(up)):
                acc = acc + dot(ref[:, pl.ds(offsets[j], size)], up[j][:, cols])
            positive = jnp.maximum(acc, 0.0)
            hidden_ref[place, cols] = (positive * positive).astype(BF)


def down_kernel(z_ref, *rest, planes):
    hidden, down, (mine_ref, other_ref) = rest[: -2 - planes], rest[-2 - planes : -2], rest[-2:]
    offsets = region_offsets(z_ref, planes, down[0].shape[1], 1)
    half = hidden[0].shape[0] // 2
    for i, ref in enumerate(hidden):
        place = pl.ds(i * half, half)
        for j, piece in enumerate(down):
            cols = pl.ds(offsets[j], piece.shape[1])
            product = dot(ref[...], piece[...]).astype(BF)
            mine_ref[place, cols] = product[:half]
            other_ref[place, cols] = product[half:]


def make_body(n_sp, n_tp):
    n_x, n_z = n_tp // 2, n_sp // 2

    def over_tp(value, turn):
        return lax.ppermute(value, "tp", [(t, turn(t)) for t in range(n_tp)])

    def over_sp(value, pairs):
        return lax.ppermute(value, "sp", pairs)

    def swap_core(value):
        return over_tp(value, lambda t: t ^ 1)

    def shift_x(value, s):
        return over_tp(value, lambda t: (t + 2 * s) % n_tp)

    def swap_y(value):
        return over_sp(value, [(i, i ^ 1) for i in range(n_sp)])

    def shift_z(value, s):
        return over_sp(value, [(i, (i + 2 * s) % n_sp) for i in range(n_sp)])

    def forward_z(value, s):
        return over_sp(value, [(i, i + 2 * s) for i in range(n_sp - 2 * s)])

    def swap_z(value):
        return over_sp(value, [(i, i ^ 2) for i in range(n_sp)])

    def body(resid, queries, keys, values, gates, log_decay, out_weight, gain, up_weight, down_weight):
        sp, tp = lax.axis_index("sp"), lax.axis_index("tp")
        y, z, core, x = sp % 2, sp // 2, tp % 2, tp // 2
        rows, heads = queries.shape[0], log_decay.shape[0]
        own_rows, width = resid.shape
        blocks = rows // BLOCK

        units = up_weight.shape[1] // 2
        same, other = (z % 2) * units, (1 - z % 2) * units
        up_same = lax.dynamic_slice_in_dim(up_weight, same, units, 1)
        up_other = lax.dynamic_slice_in_dim(up_weight, other, units, 1)
        down_same = lax.dynamic_slice_in_dim(down_weight, same, units, 0)
        down_other = lax.dynamic_slice_in_dim(down_weight, other, units, 0)
        up = [up_same] + [shift_z(up_other if s % 2 else up_same, s) for s in range(1, n_z)]
        down = [down_same] + [shift_z(down_other if s % 2 else down_same, s) for s in range(1, n_z)]
        up = up + [swap_y(piece) for piece in up]
        down = down + [swap_y(piece) for piece in down]

        inverse = 10000.0 ** (-jnp.arange(0, DK, 2, dtype=F32) / DK)
        places = jnp.concatenate(
            [jnp.arange(BLOCK, dtype=jnp.int32), sp * rows + BLOCK * jnp.arange(blocks, dtype=jnp.int32)]
        )
        angles = places[:, None].astype(F32) * inverse[None, :]
        table = jnp.stack([jnp.cos(angles), jnp.sin(angles)])
        decay = log_decay.reshape(heads, blocks, BLOCK)
        halves = 2 // heads
        size = DK // halves
        table_spec = pl.BlockSpec(table.shape, lambda h: (0, 0, 0))
        decay_spec = pl.BlockSpec((1, blocks, BLOCK), lambda h: (h, 0, 0))
        key_spec = pl.BlockSpec((rows, DK), lambda h: (0, h))
        value_spec = pl.BlockSpec((rows, DV), lambda h: (0, h))
        own_state = pl.pallas_call(
            functools.partial(state_kernel, halves=halves),
            out_shape=jax.ShapeDtypeStruct((2, size + TAIL, DV), BF),
            grid=(heads,),
            in_specs=[key_spec, value_spec, decay_spec, table_spec],
            out_specs=pl.BlockSpec((halves, size + TAIL, DV), lambda h: (h, 0, 0)),
            scratch_shapes=[pltpu.VMEM((rows, DK), BF)],
            compiler_params=params(),
            name="state",
        )(keys, values, decay, table)

        local, query_decayed = pl.pallas_call(
            local_kernel,
            out_shape=(
                jax.ShapeDtypeStruct((rows, heads * DV), F32),
                jax.ShapeDtypeStruct((rows, heads * DK), BF),
            ),
            grid=(heads,),
            in_specs=[key_spec, key_spec, value_spec, decay_spec, table_spec],
            out_specs=(value_spec, key_spec),
            scratch_shapes=[pltpu.VMEM((DK, DV), F32)],
            compiler_params=params(),
            name="local",
        )(queries, keys, values, decay, table)

        def parts(payload):
            wide = payload.astype(F32)
            return wide[size, 0] + wide[size + 1, 0], wide[:size]

        def pick(pair, index):
            return lax.dynamic_index_in_dim(pair, index, 0, keepdims=False)

        got = swap_y(pick(own_state, 1 - y))
        mine = pick(own_state, y)
        first = jnp.where(y == 0, mine, got)
        second = jnp.where(y == 0, got, mine)
        (first_decay, first_state), (second_decay, second_state) = parts(first), parts(second)
        plane_decay = first_decay * second_decay
        plane_state = second_decay * first_state + second_state
        row = lax.broadcasted_iota(jnp.int32, (TAIL, DV), 0)
        before_decay, before = jnp.ones((), F32), jnp.zeros((size, DV), F32)
        reach = 1
        while reach < n_z:
            upto_decay = before_decay * plane_decay
            upto = plane_decay * before + plane_state
            high = upto_decay.astype(BF).astype(F32)
            tail = jnp.where(row == 0, high, upto_decay - high)
            sent = forward_z(jnp.concatenate([upto, tail], axis=0).astype(BF), reach)
            far_decay, far_state = parts(sent)
            before = before_decay * far_state + before
            before_decay = before_decay * far_decay
            reach *= 2
        after_first = (first_decay * before + first_state).astype(BF)
        before = before.astype(BF)
        sent = swap_y(jnp.where(y == 0, after_first, before))
        kept = jnp.where(y == 0, before, after_first)
        incoming = jnp.stack([jnp.where(y == 0, kept, sent), jnp.where(y == 0, sent, kept)])
        incoming = incoming.reshape(heads, DK, DV)

        def projected(order):
            count = order.shape[0]
            return pl.pallas_call(
                gate_kernel,
                out_shape=jax.ShapeDtypeStruct((count, own_rows, width), BF),
                grid_spec=pltpu.PrefetchScalarGridSpec(
                    num_scalar_prefetch=1,
                    grid=(count,),
                    in_specs=[
                        pl.BlockSpec((own_rows, heads * DV), lambda j, o: (o[j], 0)),
                        pl.BlockSpec((own_rows, heads * DK), lambda j, o: (o[j], 0)),
                        pl.BlockSpec((heads, DK, DV), lambda j, o: (0, 0, 0)),
                        pl.BlockSpec((own_rows, heads * DV), lambda j, o: (o[j], 0)),
                        pl.BlockSpec(out_weight.shape, lambda j, o: (0, 0)),
                    ],
                    out_specs=pl.BlockSpec((1, own_rows, width), lambda j, o: (j, 0, 0)),
                    scratch_shapes=[pltpu.VMEM((own_rows, heads * DV), BF)],
                ),
                compiler_params=params(),
            )(order, local, query_decayed, incoming, gates, out_weight)

        def places_of(steps):
            chips = [2 * ((x + s) % n_x) for s in steps]
            return jnp.stack([c + 1 - core for c in chips] + [c + core for c in chips]).astype(jnp.int32)

        far = projected(places_of(range(1, n_x)))
        near = projected(places_of([0]))
        far_sum = (swap_core(far[: n_x - 1]).astype(F32) + far[n_x - 1 :].astype(F32)).astype(BF)
        arrived = [shift_x(far_sum[s - 1], s) for s in range(1, n_x)]
        near_other = swap_core(near[0])

        steps = max(own_rows // 128, 1)
        tall = own_rows // steps
        row_spec = pl.BlockSpec((tall, width), lambda i, o: (i, 0))
        y_word = y.astype(jnp.int32).reshape(1)
        updated, normed = pl.pallas_call(
            functools.partial(norm_kernel, regions=n_sp),
            out_shape=(jax.ShapeDtypeStruct(resid.shape, BF), jax.ShapeDtypeStruct(resid.shape, BF)),
            grid_spec=pltpu.PrefetchScalarGridSpec(
                num_scalar_prefetch=1,
                grid=(steps,),
                in_specs=[row_spec] * (3 + n_x - 1) + [pl.BlockSpec((1, width), lambda i, o: (0, 0))],
                out_specs=(row_spec, row_spec),
            ),
            compiler_params=params(),
            name="norm",
        )(y_word, resid, near[1], near_other, *arrived, gain.reshape(1, width))

        z_word = z.astype(jnp.int32).reshape(1)

        def raised(sources):
            args = (z_word, *sources, *up)
            return pl.pallas_call(
                functools.partial(up_kernel, planes=n_z, sources=len(sources)),
                out_shape=jax.ShapeDtypeStruct((2 * own_rows, units), BF),
                in_specs=[pl.BlockSpec(memory_space=pltpu.SMEM)]
                + [pl.BlockSpec(memory_space=pltpu.VMEM)] * (len(args) - 1),
                out_specs=pl.BlockSpec(memory_space=pltpu.VMEM),
                compiler_params=params(),
                name="up",
            )(*args)

        def lowered(sources, side):
            args = (z_word, *sources, *down[side * n_z : (side + 1) * n_z])
            tall = len(sources) * own_rows
            mine, others = pl.pallas_call(
                functools.partial(down_kernel, planes=n_z),
                out_shape=(jax.ShapeDtypeStruct((tall, width // 2), BF),) * 2,
                in_specs=[pl.BlockSpec(memory_space=pltpu.SMEM)]
                + [pl.BlockSpec(memory_space=pltpu.VMEM)] * (len(args) - 1),
                out_specs=(pl.BlockSpec(memory_space=pltpu.VMEM),) * 2,
                compiler_params=params(),
                name="down",
            )(*args)
            others = swap_core(others)
            parts = [slice(i * own_rows, (i + 1) * own_rows) for i in range(len(sources))]
            sums = [mine[part].astype(F32) + others[part].astype(F32) for part in parts]
            return lax.optimization_barrier(tuple(sums))

        near_x = range(1, n_x)
        top = own_rows // 2
        from_x = {s: shift_x(normed, s) for s in near_x}
        from_z = swap_z(normed)
        corner = {s: [shift_x(from_z[:top], s), swap_z(from_x[s][top:])] for s in near_x}
        chunks = {"o": [normed], "z": [from_z]}
        for s in near_x:
            chunks[f"x{s}"] = [from_x[s]]
            chunks[f"c{s}"] = corner[s]
        hidden = {key: raised(parts + [swap_core(part) for part in parts]) for key, parts in chunks.items()}
        straight = [hidden[f"x{s}"] for s in near_x] + [hidden["z"], hidden["o"]]
        corners = [hidden[f"c{s}"] for s in near_x]

        def home(value, s):
            return shift_x(value.astype(BF), n_x - s).astype(F32)

        *left_x, left_z, left_sum = lowered(straight, 0)
        left_c = lowered(corners, 0)
        *right_x, right_z, right_sum = lowered(straight, 1)
        right_c = lowered(corners, 1)
        for s in near_x:
            left_sum = left_sum + home(left_x[s - 1], s)
            left_z = left_z + home(left_c[s - 1], s)
        right_sum = right_sum + swap_z(right_z.astype(BF)).astype(F32)
        right_x = [right_x[s - 1] + swap_z(right_c[s - 1].astype(BF)).astype(F32) for s in near_x]
        left_sum = left_sum + swap_z(left_z.astype(BF)).astype(F32)
        for s in near_x:
            right_sum = right_sum + home(right_x[s - 1], s)
        pieces = [left_sum, right_sum]

        return pl.pallas_call(
            functools.partial(last_kernel, regions=n_sp),
            out_shape=jax.ShapeDtypeStruct(resid.shape, BF),
            grid_spec=pltpu.PrefetchScalarGridSpec(
                num_scalar_prefetch=1,
                grid=(steps,),
                in_specs=[row_spec] + [pl.BlockSpec((tall, width // 2), lambda i, o: (i, 0))] * 2,
                out_specs=row_spec,
            ),
            compiler_params=params(),
            name="last",
        )(y_word, updated, *pieces)

    return body


def solution(mesh):
    placed = (
        P(("sp", "tp"), None),
        P("sp", "tp"),
        P("sp", "tp"),
        P("sp", "tp"),
        P("sp", "tp"),
        P("tp", "sp"),
        P("tp", None),
        P(),
        P("sp", "tp"),
        P("tp", "sp"),
    )
    n_sp, n_tp = mesh.shape["sp"], mesh.shape["tp"]
    body = make_body(n_sp, n_tp)

    return jax.shard_map(body, mesh=mesh, in_specs=placed, out_specs=P(("sp", "tp"), None), check_vma=False)
```

```python
import functools

import jax
import jax.numpy as jnp
from jax import lax
from jax.experimental import pallas as pl
from jax.experimental.pallas import tpu as pltpu
from jax.sharding import PartitionSpec as P


DK = 256
DV = 512
BLOCK = 128
EPS = 1e-06
BF = jnp.bfloat16
F32 = jnp.float32
TAIL = 16


def params(mib=48):
    return pltpu.CompilerParams(vmem_limit_bytes=mib * 1024 * 1024)


def dot(a, b, contract=((1,), (0,))):
    return lax.dot_general(a, b, (contract, ((), ())), preferred_element_type=F32)


def decay_sums(log_decay):
    blocks = log_decay.shape[0]
    lane = lax.broadcasted_iota(jnp.int32, (blocks, BLOCK), 1)
    row = lax.broadcasted_iota(jnp.int32, (blocks, BLOCK), 0)
    cum = log_decay
    step = 1
    while step < BLOCK:
        cum = cum + jnp.where(lane >= step, pltpu.roll(cum, step, 1), 0.0)
        step *= 2
    total = jnp.broadcast_to(cum[:, BLOCK - 1 :], (blocks, BLOCK))
    upto = total
    step = 1
    while step < blocks:
        upto = upto + jnp.where(row >= step, pltpu.roll(upto, step, 0), 0.0)
        step *= 2
    padded = jnp.concatenate([cum, jnp.zeros((BLOCK - blocks, BLOCK), F32)], axis=0)
    return cum, padded.T, total, upto - total, upto[blocks - 1 :, :]


def turned(part, n, table_ref):
    half = part.shape[1] // 2
    cos_r, sin_r = table_ref[0, :BLOCK, :], table_ref[1, :BLOCK, :]
    cos_b, sin_b = table_ref[0, BLOCK + n : BLOCK + n + 1, :], table_ref[1, BLOCK + n : BLOCK + n + 1, :]
    cosine = cos_r * cos_b - sin_r * sin_b
    sine = sin_r * cos_b + cos_r * sin_b
    first, second = part[:, :half].astype(F32), part[:, half:].astype(F32)
    return first * cosine - second * sine, first * sine + second * cosine


def with_decay(out_ref, state, decay):
    size = state.shape[0]
    high = decay.astype(BF).astype(F32)
    row = lax.broadcasted_iota(jnp.int32, (TAIL, DV), 0)
    out_ref[:size, :] = state.astype(BF)
    out_ref[size:, :] = jnp.where(row == 0, high, decay - high).astype(BF)


def parts_of(payload):
    size = payload.shape[0] - TAIL
    wide = payload.astype(F32)
    return wide[size : size + 1, :] + wide[size + 1 : size + 2, :], wide[:size, :]


def state_kernel(y_ref, key_ref, value_ref, decay_ref, table_ref, mine_ref, theirs_ref, kd_ref, *, halves):
    blocks = decay_ref.shape[1]
    _, col, _, before, whole = decay_sums(decay_ref[0])
    scale = DK ** (-0.5)
    for n in range(blocks):
        rows = pl.ds(n * BLOCK, BLOCK)
        a, b = turned(key_ref[rows, :], n, table_ref)
        a, b = (a * scale).astype(BF).astype(F32), (b * scale).astype(BF).astype(F32)
        factor = jnp.exp(whole - before[n : n + 1, :] - jnp.broadcast_to(col[:, n : n + 1], (BLOCK, BLOCK)))
        kd_ref[rows, : DK // 2] = (a * factor).astype(BF)
        kd_ref[rows, DK // 2 :] = (b * factor).astype(BF)
    state = dot(kd_ref[...], value_ref[...], ((0,), (0,)))
    decay = jnp.broadcast_to(jnp.exp(whole[:, :1]), (1, DV))
    size = DK // halves
    for j in range(halves):
        half = pl.program_id(0) * halves + j

        @pl.when(half == y_ref[0])
        def _():
            with_decay(mine_ref, state[j * size : (j + 1) * size, :], decay)

        @pl.when(half != y_ref[0])
        def _():
            with_decay(theirs_ref, state[j * size : (j + 1) * size, :], decay)


def in_order(y_ref, mine_ref, got_ref):
    (mine_decay, mine), (got_decay, got) = parts_of(mine_ref[...]), parts_of(got_ref[...])
    lower = y_ref[0] == 0
    return (
        (jnp.where(lower, mine_decay, got_decay), jnp.where(lower, mine, got)),
        (jnp.where(lower, got_decay, mine_decay), jnp.where(lower, got, mine)),
    )


def before_of(sent):
    decay, before = parts_of(sent[0][...])
    for ref in sent[1:]:
        far_decay, far_state = parts_of(ref[...])
        before = decay * far_state + before
        decay = decay * far_decay
    return decay, before


def plane_kernel(y_ref, mine_ref, got_ref, out_ref):
    (first_decay, first), (second_decay, second) = in_order(y_ref, mine_ref, got_ref)
    with_decay(out_ref, second_decay * first + second, second_decay * first_decay)


def upto_kernel(plane_ref, *rest):
    sent, out_ref = rest[:-1], rest[-1]
    decay, before = before_of(sent)
    plane_decay, plane = parts_of(plane_ref[...])
    with_decay(out_ref, plane_decay * before + plane, plane_decay * decay)


def before_kernel(y_ref, mine_ref, got_ref, *rest):
    sent, (send_ref, keep_ref) = rest[:-2], rest[-2:]
    (first_decay, first), _ = in_order(y_ref, mine_ref, got_ref)
    before = before_of(sent)[1]
    after = first_decay * before + first
    lower = y_ref[0] == 0
    send_ref[...] = jnp.where(lower, after, before).astype(BF)
    keep_ref[...] = jnp.where(lower, before, after).astype(BF)


def local_kernel(query_ref, key_ref, value_ref, decay_ref, table_ref, out_ref, qd_ref, state_ref):
    blocks = decay_ref.shape[1]
    cum, col, total, before, _ = decay_sums(decay_ref[0])
    scale = DK ** (-0.5)
    causal = lax.broadcasted_iota(jnp.int32, (BLOCK, BLOCK), 0) >= lax.broadcasted_iota(
        jnp.int32, (BLOCK, BLOCK), 1
    )
    for n in range(blocks):
        rows = pl.ds(n * BLOCK, BLOCK)
        qa, qb = turned(query_ref[rows, :], n, table_ref)
        ka, kb = turned(key_ref[rows, :], n, table_ref)
        qa, qb = qa.astype(BF), qb.astype(BF)
        ka, kb = (ka * scale).astype(BF), (kb * scale).astype(BF)
        query = jnp.concatenate([qa, qb], axis=1)
        key = jnp.concatenate([ka, kb], axis=1)
        value = value_ref[rows, :]
        down = jnp.broadcast_to(col[:, n : n + 1], (BLOCK, BLOCK))
        spread = down - cum[n : n + 1, :]
        factor = jnp.where(causal, jnp.exp(jnp.minimum(spread, 0.0)), 0.0)
        weights = (dot(query, key, ((1,), (1,))) * factor).astype(BF)
        result = dot(weights, value)
        from_block = jnp.exp(down)
        if n:
            near = jnp.concatenate(
                [(qa.astype(F32) * from_block).astype(BF), (qb.astype(F32) * from_block).astype(BF)], axis=1
            )
            result = result + dot(near, state_ref[...].astype(BF))
        out_ref[rows, :] = result
        from_start = jnp.exp(down + before[n : n + 1, :])
        qd_ref[rows, : DK // 2] = (qa.astype(F32) * from_start).astype(BF)
        qd_ref[rows, DK // 2 :] = (qb.astype(F32) * from_start).astype(BF)
        if n + 1 < blocks:
            to_end = jnp.exp(total[n : n + 1, :] - down)
            kd = jnp.concatenate(
                [(ka.astype(F32) * to_end).astype(BF), (kb.astype(F32) * to_end).astype(BF)], axis=1
            )
            term = dot(kd, value, ((0,), (0,)))
            if n:
                state_ref[...] = jnp.exp(total[n : n + 1, :1]) * state_ref[...] + term
            else:
                state_ref[...] = term


def gate_kernel(order_ref, y_ref, local_ref, qd_ref, keep_ref, sent_ref, gate_ref, weight_ref, out_ref, gated_ref, in_ref):
    heads = local_ref.shape[1] // DV
    size = keep_ref.shape[0]

    @pl.when(pl.program_id(0) == 0)
    def _():
        in_ref[y_ref[0]] = keep_ref[...]
        in_ref[1 - y_ref[0]] = sent_ref[...]

    for h in range(heads):
        cols = pl.ds(h * DV, DV)
        retained = local_ref[:, cols]
        for j in range(h * DK // size, (h + 1) * DK // size):
            retained = retained + dot(qd_ref[:, pl.ds(j * size, size)], in_ref[j])
        mean = jnp.mean(retained * retained, axis=-1, keepdims=True)
        gate = gate_ref[:, cols].astype(F32)
        silu = gate / (1.0 + jnp.exp(-gate))
        gated_ref[:, cols] = (silu * (retained * lax.rsqrt(mean + EPS))).astype(BF)
    out_ref[0] = dot(gated_ref[...], weight_ref[...]).astype(BF)


def norm_kernel(y_ref, resid_ref, a_ref, b_ref, *rest, regions):
    far, (gain_ref, updated_ref, normed_ref) = rest[:-3], rest[-3:]
    mixed = a_ref[...].astype(F32) + b_ref[...].astype(F32)
    for ref in far:
        mixed = mixed + ref[...].astype(F32)
    updated = (resid_ref[...].astype(F32) + mixed).astype(BF)
    updated_ref[...] = updated
    wide = updated.astype(F32)
    scaled = wide * lax.rsqrt(jnp.mean(wide * wide, axis=-1, keepdims=True) + EPS)
    normed = (scaled * gain_ref[...].astype(F32)).astype(BF)
    size = normed.shape[1] // regions
    half = regions // 2
    lower = y_ref[0] == 0
    for r in range(half):
        even = normed[:, 2 * r * size : (2 * r + 1) * size]
        odd = normed[:, (2 * r + 1) * size : (2 * r + 2) * size]
        normed_ref[:, r * size : (r + 1) * size] = jnp.where(lower, even, odd)
        normed_ref[:, (half + r) * size : (half + r + 1) * size] = jnp.where(lower, odd, even)


def last_kernel(y_ref, updated_ref, *rest, regions):
    left_ref, right_ref, out_ref = rest
    size = 2 * left_ref.shape[1] // regions
    half = regions // 2
    lower = y_ref[0] == 0
    for r in range(half):
        own = left_ref[:, r * size : (r + 1) * size]
        other = right_ref[:, r * size : (r + 1) * size]
        even, odd = pl.ds(2 * r * size, size), pl.ds((2 * r + 1) * size, size)
        out_ref[:, even] = (updated_ref[:, even].astype(F32) + jnp.where(lower, own, other)).astype(BF)
        out_ref[:, odd] = (updated_ref[:, odd].astype(F32) + jnp.where(lower, other, own)).astype(BF)


def region_offsets(z_ref, planes, size, sides):
    offsets = []
    for side in range(sides):
        for s in range(planes):
            plane = lax.rem(z_ref[0] + (planes - s), planes)
            offsets.append(pl.multiple_of((side * planes + plane) * size, size))
    return offsets


def up_kernel(z_ref, *rest, planes, sources):
    rows, up, hidden_ref = rest[:sources], rest[sources:-1], rest[-1]
    size, units = up[0].shape
    offsets = region_offsets(z_ref, planes, size, 2)
    chunk = min(256, units)
    start = 0
    for ref in rows:
        place = pl.ds(start, ref.shape[0])
        start += ref.shape[0]
        for c in range(units // chunk):
            cols = pl.ds(c * chunk, chunk)
            acc = dot(ref[:, pl.ds(offsets[0], size)], up[0][:, cols])
            for j in range(1, len(up)):
                acc = acc + dot(ref[:, pl.ds(offsets[j], size)], up[j][:, cols])
            positive = jnp.maximum(acc, 0.0)
            hidden_ref[place, cols] = (positive * positive).astype(BF)


def down_kernel(z_ref, *rest, planes):
    hidden, down, (mine_ref, other_ref) = rest[: -2 - planes], rest[-2 - planes : -2], rest[-2:]
    offsets = region_offsets(z_ref, planes, down[0].shape[1], 1)
    half = hidden[0].shape[0] // 2
    for i, ref in enumerate(hidden):
        place = pl.ds(i * half, half)
        for j, piece in enumerate(down):
            cols = pl.ds(offsets[j], piece.shape[1])
            product = dot(ref[...], piece[...]).astype(BF)
            mine_ref[place, cols] = product[:half]
            other_ref[place, cols] = product[half:]


def make_body(n_sp, n_tp):
    n_x, n_z = n_tp // 2, n_sp // 2

    def over_tp(value, turn):
        return lax.ppermute(value, "tp", [(t, turn(t)) for t in range(n_tp)])

    def over_sp(value, pairs):
        return lax.ppermute(value, "sp", pairs)

    def swap_core(value):
        return over_tp(value, lambda t: t ^ 1)

    def shift_x(value, s):
        return over_tp(value, lambda t: (t + 2 * s) % n_tp)

    def swap_y(value):
        return over_sp(value, [(i, i ^ 1) for i in range(n_sp)])

    def shift_z(value, s):
        return over_sp(value, [(i, (i + 2 * s) % n_sp) for i in range(n_sp)])

    def forward_z(value, s):
        return over_sp(value, [(i, i + 2 * s) for i in range(n_sp - 2 * s)])

    def swap_z(value):
        return over_sp(value, [(i, i ^ 2) for i in range(n_sp)])

    def body(resid, queries, keys, values, gates, log_decay, out_weight, gain, up_weight, down_weight):
        sp, tp = lax.axis_index("sp"), lax.axis_index("tp")
        y, z, core, x = sp % 2, sp // 2, tp % 2, tp // 2
        rows, heads = queries.shape[0], log_decay.shape[0]
        own_rows, width = resid.shape
        blocks = rows // BLOCK

        units = up_weight.shape[1] // 2
        same, other = (z % 2) * units, (1 - z % 2) * units
        up_same = lax.dynamic_slice_in_dim(up_weight, same, units, 1)
        up_other = lax.dynamic_slice_in_dim(up_weight, other, units, 1)
        down_same = lax.dynamic_slice_in_dim(down_weight, same, units, 0)
        down_other = lax.dynamic_slice_in_dim(down_weight, other, units, 0)
        up = [up_same] + [shift_z(up_other if s % 2 else up_same, s) for s in range(1, n_z)]
        down = [down_same] + [shift_z(down_other if s % 2 else down_same, s) for s in range(1, n_z)]
        up = up + [swap_y(piece) for piece in up]
        down = down + [swap_y(piece) for piece in down]

        inverse = 10000.0 ** (-jnp.arange(0, DK, 2, dtype=F32) / DK)
        places = jnp.concatenate(
            [jnp.arange(BLOCK, dtype=jnp.int32), sp * rows + BLOCK * jnp.arange(blocks, dtype=jnp.int32)]
        )
        angles = places[:, None].astype(F32) * inverse[None, :]
        table = jnp.stack([jnp.cos(angles), jnp.sin(angles)])
        decay = log_decay.reshape(heads, blocks, BLOCK)
        halves = 2 // heads
        size = DK // halves
        table_spec = pl.BlockSpec(table.shape, lambda h: (0, 0, 0))
        decay_spec = pl.BlockSpec((1, blocks, BLOCK), lambda h: (h, 0, 0))
        key_spec = pl.BlockSpec((rows, DK), lambda h: (0, h))
        value_spec = pl.BlockSpec((rows, DV), lambda h: (0, h))
        y_word = y.astype(jnp.int32).reshape(1)
        payload = jax.ShapeDtypeStruct((size + TAIL, DV), BF)
        payload_spec = pl.BlockSpec(payload.shape, lambda h: (0, 0))
        word_spec = pl.BlockSpec(memory_space=pltpu.SMEM)
        mine, theirs = pl.pallas_call(
            functools.partial(state_kernel, halves=halves),
            out_shape=(payload, payload),
            grid=(heads,),
            in_specs=[word_spec, key_spec, value_spec, decay_spec, table_spec],
            out_specs=(payload_spec, payload_spec),
            scratch_shapes=[pltpu.VMEM((rows, DK), BF)],
            compiler_params=params(),
            name="state",
        )(y_word, keys, values, decay, table)

        local, query_decayed = pl.pallas_call(
            local_kernel,
            out_shape=(
                jax.ShapeDtypeStruct((rows, heads * DV), F32),
                jax.ShapeDtypeStruct((rows, heads * DK), BF),
            ),
            grid=(heads,),
            in_specs=[key_spec, key_spec, value_spec, decay_spec, table_spec],
            out_specs=(value_spec, key_spec),
            scratch_shapes=[pltpu.VMEM((DK, DV), F32)],
            compiler_params=params(),
            name="local",
        )(queries, keys, values, decay, table)

        def small(kernel, out_shape, *args):
            return pl.pallas_call(
                kernel,
                out_shape=out_shape,
                in_specs=[word_spec if arg is y_word else pl.BlockSpec(memory_space=pltpu.VMEM) for arg in args],
                compiler_params=params(),
            )(*args)

        got = swap_y(theirs)
        plane = upto = small(plane_kernel, payload, y_word, mine, got)
        sent = [forward_z(plane, 1)]
        reach = 2
        while reach < n_z:
            upto = small(upto_kernel, payload, plane, *sent)
            sent.append(forward_z(upto, reach))
            reach *= 2
        state_half = jax.ShapeDtypeStruct((size, DV), BF)
        send, keep = small(before_kernel, (state_half, state_half), y_word, mine, got, *sent)
        arrived_state = swap_y(send)

        def projected(order):
            count = order.shape[0]
            return pl.pallas_call(
                gate_kernel,
                out_shape=jax.ShapeDtypeStruct((count, own_rows, width), BF),
                grid_spec=pltpu.PrefetchScalarGridSpec(
                    num_scalar_prefetch=2,
                    grid=(count,),
                    in_specs=[
                        pl.BlockSpec((own_rows, heads * DV), lambda j, o, w: (o[j], 0)),
                        pl.BlockSpec((own_rows, heads * DK), lambda j, o, w: (o[j], 0)),
                        pl.BlockSpec((size, DV), lambda j, o, w: (0, 0)),
                        pl.BlockSpec((size, DV), lambda j, o, w: (0, 0)),
                        pl.BlockSpec((own_rows, heads * DV), lambda j, o, w: (o[j], 0)),
                        pl.BlockSpec(out_weight.shape, lambda j, o, w: (0, 0)),
                    ],
                    out_specs=pl.BlockSpec((1, own_rows, width), lambda j, o, w: (j, 0, 0)),
                    scratch_shapes=[pltpu.VMEM((own_rows, heads * DV), BF), pltpu.VMEM((2, size, DV), BF)],
                ),
                compiler_params=params(),
            )(order, y_word, local, query_decayed, keep, arrived_state, gates, out_weight)

        def places_of(steps):
            chips = [2 * ((x + s) % n_x) for s in steps]
            return jnp.stack([c + 1 - core for c in chips] + [c + core for c in chips]).astype(jnp.int32)

        far = projected(places_of(range(1, n_x)))
        near = projected(places_of([0]))
        far_sum = (swap_core(far[: n_x - 1]).astype(F32) + far[n_x - 1 :].astype(F32)).astype(BF)
        arrived = [shift_x(far_sum[s - 1], s) for s in range(1, n_x)]
        near_other = swap_core(near[0])

        steps = max(own_rows // 128, 1)
        tall = own_rows // steps
        row_spec = pl.BlockSpec((tall, width), lambda i, o: (i, 0))
        updated, normed = pl.pallas_call(
            functools.partial(norm_kernel, regions=n_sp),
            out_shape=(jax.ShapeDtypeStruct(resid.shape, BF), jax.ShapeDtypeStruct(resid.shape, BF)),
            grid_spec=pltpu.PrefetchScalarGridSpec(
                num_scalar_prefetch=1,
                grid=(steps,),
                in_specs=[row_spec] * (3 + n_x - 1) + [pl.BlockSpec((1, width), lambda i, o: (0, 0))],
                out_specs=(row_spec, row_spec),
            ),
            compiler_params=params(),
            name="norm",
        )(y_word, resid, near[1], near_other, *arrived, gain.reshape(1, width))

        z_word = z.astype(jnp.int32).reshape(1)

        def raised(sources):
            args = (z_word, *sources, *up)
            return pl.pallas_call(
                functools.partial(up_kernel, planes=n_z, sources=len(sources)),
                out_shape=jax.ShapeDtypeStruct((2 * own_rows, units), BF),
                in_specs=[pl.BlockSpec(memory_space=pltpu.SMEM)]
                + [pl.BlockSpec(memory_space=pltpu.VMEM)] * (len(args) - 1),
                out_specs=pl.BlockSpec(memory_space=pltpu.VMEM),
                compiler_params=params(),
                name="up",
            )(*args)

        def lowered(sources, side):
            args = (z_word, *sources, *down[side * n_z : (side + 1) * n_z])
            tall = len(sources) * own_rows
            mine, others = pl.pallas_call(
                functools.partial(down_kernel, planes=n_z),
                out_shape=(jax.ShapeDtypeStruct((tall, width // 2), BF),) * 2,
                in_specs=[pl.BlockSpec(memory_space=pltpu.SMEM)]
                + [pl.BlockSpec(memory_space=pltpu.VMEM)] * (len(args) - 1),
                out_specs=(pl.BlockSpec(memory_space=pltpu.VMEM),) * 2,
                compiler_params=params(),
                name="down",
            )(*args)
            others = swap_core(others)
            parts = [slice(i * own_rows, (i + 1) * own_rows) for i in range(len(sources))]
            sums = [mine[part].astype(F32) + others[part].astype(F32) for part in parts]
            return lax.optimization_barrier(tuple(sums))

        near_x = range(1, n_x)
        top = own_rows // 2
        upper, under = normed[:top], normed[top:]
        x_under = {s: shift_x(under, s) for s in near_x}
        z_upper = swap_z(upper)
        x_upper = {s: shift_x(upper, s) for s in near_x}
        z_under = swap_z(under)
        chunks = {"o": [normed], "z": [z_upper, z_under]}
        for s in near_x:
            chunks[f"x{s}"] = [x_upper[s], x_under[s]]
            chunks[f"c{s}"] = [shift_x(z_upper, s), swap_z(x_under[s])]
        hidden = {key: raised(parts + [swap_core(part) for part in parts]) for key, parts in chunks.items()}
        straight = [hidden[f"x{s}"] for s in near_x] + [hidden["z"], hidden["o"]]
        corners = [hidden[f"c{s}"] for s in near_x]

        def home(value, s):
            return shift_x(value.astype(BF), n_x - s).astype(F32)

        (left_z,) = lowered([hidden["z"]], 0)
        *left_x, left_sum = lowered(straight[:-2] + straight[-1:], 0)
        left_c = lowered(corners, 0)
        (right_z,) = lowered([hidden["z"]], 1)
        *right_x, right_sum = lowered(straight[:-2] + straight[-1:], 1)
        right_c = lowered(corners, 1)
        for s in near_x:
            left_sum = left_sum + home(left_x[s - 1], s)
            left_z = left_z + home(left_c[s - 1], s)
        right_sum = right_sum + swap_z(right_z.astype(BF)).astype(F32)
        right_x = [right_x[s - 1] + swap_z(right_c[s - 1].astype(BF)).astype(F32) for s in near_x]
        left_sum = left_sum + swap_z(left_z.astype(BF)).astype(F32)
        for s in near_x:
            right_sum = right_sum + home(right_x[s - 1], s)
        pieces = [left_sum, right_sum]

        return pl.pallas_call(
            functools.partial(last_kernel, regions=n_sp),
            out_shape=jax.ShapeDtypeStruct(resid.shape, BF),
            grid_spec=pltpu.PrefetchScalarGridSpec(
                num_scalar_prefetch=1,
                grid=(steps,),
                in_specs=[row_spec] + [pl.BlockSpec((tall, width // 2), lambda i, o: (i, 0))] * 2,
                out_specs=row_spec,
            ),
            compiler_params=params(),
            name="last",
        )(y_word, updated, *pieces)

    return body


def solution(mesh):
    placed = (
        P(("sp", "tp"), None),
        P("sp", "tp"),
        P("sp", "tp"),
        P("sp", "tp"),
        P("sp", "tp"),
        P("tp", "sp"),
        P("tp", None),
        P(),
        P("sp", "tp"),
        P("tp", "sp"),
    )
    n_sp, n_tp = mesh.shape["sp"], mesh.shape["tp"]
    body = make_body(n_sp, n_tp)

    return jax.shard_map(body, mesh=mesh, in_specs=placed, out_specs=P(("sp", "tp"), None), check_vma=False)
```

```python
import functools

import jax
import jax.numpy as jnp
from jax import lax
from jax.experimental import pallas as pl
from jax.experimental.pallas import tpu as pltpu
from jax.sharding import PartitionSpec as P


DK = 256
DV = 512
BLOCK = 128
EPS = 1e-06
BF = jnp.bfloat16
F32 = jnp.float32
TAIL = 16


def params(mib=48):
    return pltpu.CompilerParams(vmem_limit_bytes=mib * 1024 * 1024)


def dot(a, b, contract=((1,), (0,))):
    return lax.dot_general(a, b, (contract, ((), ())), preferred_element_type=F32)


def decay_sums(log_decay):
    blocks = log_decay.shape[0]
    lane = lax.broadcasted_iota(jnp.int32, (blocks, BLOCK), 1)
    row = lax.broadcasted_iota(jnp.int32, (blocks, BLOCK), 0)
    cum = log_decay
    step = 1
    while step < BLOCK:
        cum = cum + jnp.where(lane >= step, pltpu.roll(cum, step, 1), 0.0)
        step *= 2
    total = jnp.broadcast_to(cum[:, BLOCK - 1 :], (blocks, BLOCK))
    upto = total
    step = 1
    while step < blocks:
        upto = upto + jnp.where(row >= step, pltpu.roll(upto, step, 0), 0.0)
        step *= 2
    padded = jnp.concatenate([cum, jnp.zeros((BLOCK - blocks, BLOCK), F32)], axis=0)
    return cum, padded.T, total, upto - total, upto[blocks - 1 :, :]


def turned(part, n, table_ref):
    half = part.shape[1] // 2
    cos_r, sin_r = table_ref[0, :BLOCK, :], table_ref[1, :BLOCK, :]
    cos_b, sin_b = table_ref[0, BLOCK + n : BLOCK + n + 1, :], table_ref[1, BLOCK + n : BLOCK + n + 1, :]
    cosine = cos_r * cos_b - sin_r * sin_b
    sine = sin_r * cos_b + cos_r * sin_b
    first, second = part[:, :half].astype(F32), part[:, half:].astype(F32)
    return first * cosine - second * sine, first * sine + second * cosine


def with_decay(out_ref, state, decay):
    size = state.shape[0]
    high = decay.astype(BF).astype(F32)
    row = lax.broadcasted_iota(jnp.int32, (TAIL, DV), 0)
    out_ref[:size, :] = state.astype(BF)
    out_ref[size:, :] = jnp.where(row == 0, high, decay - high).astype(BF)


def parts_of(payload):
    size = payload.shape[0] - TAIL
    wide = payload.astype(F32)
    return wide[size : size + 1, :] + wide[size + 1 : size + 2, :], wide[:size, :]


def state_kernel(y_ref, key_ref, value_ref, decay_ref, table_ref, mine_ref, theirs_ref, kd_ref, *, halves):
    blocks = decay_ref.shape[1]
    _, col, _, before, whole = decay_sums(decay_ref[0])
    scale = DK ** (-0.5)
    for n in range(blocks):
        rows = pl.ds(n * BLOCK, BLOCK)
        a, b = turned(key_ref[rows, :], n, table_ref)
        a, b = (a * scale).astype(BF).astype(F32), (b * scale).astype(BF).astype(F32)
        factor = jnp.exp(whole - before[n : n + 1, :] - jnp.broadcast_to(col[:, n : n + 1], (BLOCK, BLOCK)))
        kd_ref[rows, : DK // 2] = (a * factor).astype(BF)
        kd_ref[rows, DK // 2 :] = (b * factor).astype(BF)
    state = dot(kd_ref[...], value_ref[...], ((0,), (0,)))
    decay = jnp.broadcast_to(jnp.exp(whole[:, :1]), (1, DV))
    size = DK // halves
    for j in range(halves):
        half = pl.program_id(0) * halves + j

        @pl.when(half == y_ref[0])
        def _():
            with_decay(mine_ref, state[j * size : (j + 1) * size, :], decay)

        @pl.when(half != y_ref[0])
        def _():
            with_decay(theirs_ref, state[j * size : (j + 1) * size, :], decay)


def in_order(y_ref, mine_ref, got_ref):
    (mine_decay, mine), (got_decay, got) = parts_of(mine_ref[...]), parts_of(got_ref[...])
    lower = y_ref[0] == 0
    return (
        (jnp.where(lower, mine_decay, got_decay), jnp.where(lower, mine, got)),
        (jnp.where(lower, got_decay, mine_decay), jnp.where(lower, got, mine)),
    )


def before_of(sent):
    decay, before = parts_of(sent[0][...])
    for ref in sent[1:]:
        far_decay, far_state = parts_of(ref[...])
        before = decay * far_state + before
        decay = decay * far_decay
    return decay, before


def plane_kernel(y_ref, mine_ref, got_ref, out_ref):
    (first_decay, first), (second_decay, second) = in_order(y_ref, mine_ref, got_ref)
    with_decay(out_ref, second_decay * first + second, second_decay * first_decay)


def upto_kernel(plane_ref, *rest):
    sent, out_ref = rest[:-1], rest[-1]
    decay, before = before_of(sent)
    plane_decay, plane = parts_of(plane_ref[...])
    with_decay(out_ref, plane_decay * before + plane, plane_decay * decay)


def before_kernel(y_ref, mine_ref, got_ref, *rest):
    sent, (send_ref, keep_ref) = rest[:-2], rest[-2:]
    (first_decay, first), _ = in_order(y_ref, mine_ref, got_ref)
    before = before_of(sent)[1]
    after = first_decay * before + first
    lower = y_ref[0] == 0
    send_ref[...] = jnp.where(lower, after, before).astype(BF)
    keep_ref[...] = jnp.where(lower, before, after).astype(BF)


def local_kernel(query_ref, key_ref, value_ref, decay_ref, table_ref, out_ref, qd_ref, state_ref):
    blocks = decay_ref.shape[1]
    cum, col, total, before, _ = decay_sums(decay_ref[0])
    scale = DK ** (-0.5)
    causal = lax.broadcasted_iota(jnp.int32, (BLOCK, BLOCK), 0) >= lax.broadcasted_iota(
        jnp.int32, (BLOCK, BLOCK), 1
    )
    for n in range(blocks):
        rows = pl.ds(n * BLOCK, BLOCK)
        qa, qb = turned(query_ref[rows, :], n, table_ref)
        ka, kb = turned(key_ref[rows, :], n, table_ref)
        qa, qb = qa.astype(BF), qb.astype(BF)
        ka, kb = (ka * scale).astype(BF), (kb * scale).astype(BF)
        query = jnp.concatenate([qa, qb], axis=1)
        key = jnp.concatenate([ka, kb], axis=1)
        value = value_ref[rows, :]
        down = jnp.broadcast_to(col[:, n : n + 1], (BLOCK, BLOCK))
        spread = down - cum[n : n + 1, :]
        factor = jnp.where(causal, jnp.exp(jnp.minimum(spread, 0.0)), 0.0)
        weights = (dot(query, key, ((1,), (1,))) * factor).astype(BF)
        result = dot(weights, value)
        from_block = jnp.exp(down)
        if n:
            near = jnp.concatenate(
                [(qa.astype(F32) * from_block).astype(BF), (qb.astype(F32) * from_block).astype(BF)], axis=1
            )
            result = result + dot(near, state_ref[...].astype(BF))
        out_ref[rows, :] = result
        from_start = jnp.exp(down + before[n : n + 1, :])
        qd_ref[rows, : DK // 2] = (qa.astype(F32) * from_start).astype(BF)
        qd_ref[rows, DK // 2 :] = (qb.astype(F32) * from_start).astype(BF)
        if n + 1 < blocks:
            to_end = jnp.exp(total[n : n + 1, :] - down)
            kd = jnp.concatenate(
                [(ka.astype(F32) * to_end).astype(BF), (kb.astype(F32) * to_end).astype(BF)], axis=1
            )
            term = dot(kd, value, ((0,), (0,)))
            if n:
                state_ref[...] = jnp.exp(total[n : n + 1, :1]) * state_ref[...] + term
            else:
                state_ref[...] = term


def gate_kernel(order_ref, y_ref, local_ref, qd_ref, keep_ref, sent_ref, gate_ref, weight_ref, out_ref, gated_ref, in_ref):
    heads = local_ref.shape[1] // DV
    size = keep_ref.shape[0]

    @pl.when(pl.program_id(0) == 0)
    def _():
        in_ref[y_ref[0]] = keep_ref[...]
        in_ref[1 - y_ref[0]] = sent_ref[...]

    for h in range(heads):
        cols = pl.ds(h * DV, DV)
        retained = local_ref[:, cols]
        for j in range(h * DK // size, (h + 1) * DK // size):
            retained = retained + dot(qd_ref[:, pl.ds(j * size, size)], in_ref[j])
        mean = jnp.mean(retained * retained, axis=-1, keepdims=True)
        gate = gate_ref[:, cols].astype(F32)
        silu = gate / (1.0 + jnp.exp(-gate))
        gated_ref[:, cols] = (silu * (retained * lax.rsqrt(mean + EPS))).astype(BF)
    out_ref[0] = dot(gated_ref[...], weight_ref[...]).astype(BF)


def norm_kernel(y_ref, resid_ref, a_ref, b_ref, *rest, regions):
    far, (gain_ref, updated_ref, normed_ref) = rest[:-3], rest[-3:]
    mixed = a_ref[...].astype(F32) + b_ref[...].astype(F32)
    for ref in far:
        mixed = mixed + ref[...].astype(F32)
    updated = (resid_ref[...].astype(F32) + mixed).astype(BF)
    updated_ref[...] = updated
    wide = updated.astype(F32)
    scaled = wide * lax.rsqrt(jnp.mean(wide * wide, axis=-1, keepdims=True) + EPS)
    normed = (scaled * gain_ref[...].astype(F32)).astype(BF)
    size = normed.shape[1] // regions
    half = regions // 2
    lower = y_ref[0] == 0
    for r in range(half):
        even = normed[:, 2 * r * size : (2 * r + 1) * size]
        odd = normed[:, (2 * r + 1) * size : (2 * r + 2) * size]
        normed_ref[:, r * size : (r + 1) * size] = jnp.where(lower, even, odd)
        normed_ref[:, (half + r) * size : (half + r + 1) * size] = jnp.where(lower, odd, even)


def last_kernel(y_ref, updated_ref, *rest, regions):
    left_ref, right_ref, out_ref = rest
    size = 2 * left_ref.shape[1] // regions
    half = regions // 2
    lower = y_ref[0] == 0
    for r in range(half):
        own = left_ref[:, r * size : (r + 1) * size]
        other = right_ref[:, r * size : (r + 1) * size]
        even, odd = pl.ds(2 * r * size, size), pl.ds((2 * r + 1) * size, size)
        out_ref[:, even] = (updated_ref[:, even].astype(F32) + jnp.where(lower, own, other)).astype(BF)
        out_ref[:, odd] = (updated_ref[:, odd].astype(F32) + jnp.where(lower, other, own)).astype(BF)


def region_offsets(z_ref, planes, size, sides):
    offsets = []
    for side in range(sides):
        for s in range(planes):
            plane = lax.rem(z_ref[0] + (planes - s), planes)
            offsets.append(pl.multiple_of((side * planes + plane) * size, size))
    return offsets


def up_kernel(z_ref, *rest, planes, sources):
    rows, up, hidden_ref = rest[:sources], rest[sources:-1], rest[-1]
    size, units = up[0].shape
    offsets = region_offsets(z_ref, planes, size, 2)
    chunk = min(256, units)
    start = 0
    for ref in rows:
        place = pl.ds(start, ref.shape[0])
        start += ref.shape[0]
        for c in range(units // chunk):
            cols = pl.ds(c * chunk, chunk)
            acc = dot(ref[:, pl.ds(offsets[0], size)], up[0][:, cols])
            for j in range(1, len(up)):
                acc = acc + dot(ref[:, pl.ds(offsets[j], size)], up[j][:, cols])
            positive = jnp.maximum(acc, 0.0)
            hidden_ref[place, cols] = (positive * positive).astype(BF)


def down_kernel(z_ref, *rest, planes):
    hidden, down, (mine_ref, other_ref) = rest[: -2 - planes], rest[-2 - planes : -2], rest[-2:]
    offsets = region_offsets(z_ref, planes, down[0].shape[1], 1)
    half = hidden[0].shape[0] // 2
    for i, ref in enumerate(hidden):
        place = pl.ds(i * half, half)
        for j, piece in enumerate(down):
            cols = pl.ds(offsets[j], piece.shape[1])
            product = dot(ref[...], piece[...]).astype(BF)
            mine_ref[place, cols] = product[:half]
            other_ref[place, cols] = product[half:]


def make_body(n_sp, n_tp):
    n_x, n_z = n_tp // 2, n_sp // 2

    def over_tp(value, turn):
        return lax.ppermute(value, "tp", [(t, turn(t)) for t in range(n_tp)])

    def over_sp(value, pairs):
        return lax.ppermute(value, "sp", pairs)

    def swap_core(value):
        return over_tp(value, lambda t: t ^ 1)

    def shift_x(value, s):
        return over_tp(value, lambda t: (t + 2 * s) % n_tp)

    def swap_y(value):
        return over_sp(value, [(i, i ^ 1) for i in range(n_sp)])

    def shift_z(value, s):
        return over_sp(value, [(i, (i + 2 * s) % n_sp) for i in range(n_sp)])

    def forward_z(value, s):
        return over_sp(value, [(i, i + 2 * s) for i in range(n_sp - 2 * s)])

    def swap_z(value):
        return over_sp(value, [(i, i ^ 2) for i in range(n_sp)])

    def body(resid, queries, keys, values, gates, log_decay, out_weight, gain, up_weight, down_weight):
        sp, tp = lax.axis_index("sp"), lax.axis_index("tp")
        y, z, core, x = sp % 2, sp // 2, tp % 2, tp // 2
        rows, heads = queries.shape[0], log_decay.shape[0]
        own_rows, width = resid.shape
        blocks = rows // BLOCK

        units = up_weight.shape[1] // 2
        same, other = (z % 2) * units, (1 - z % 2) * units
        up_same = lax.dynamic_slice_in_dim(up_weight, same, units, 1)
        up_other = lax.dynamic_slice_in_dim(up_weight, other, units, 1)
        down_same = lax.dynamic_slice_in_dim(down_weight, same, units, 0)
        down_other = lax.dynamic_slice_in_dim(down_weight, other, units, 0)
        up = [up_same] + [shift_z(up_other if s % 2 else up_same, s) for s in range(1, n_z)]
        down = [down_same] + [shift_z(down_other if s % 2 else down_same, s) for s in range(1, n_z)]
        up = up + [swap_y(piece) for piece in up]
        down = down + [swap_y(piece) for piece in down]

        inverse = 10000.0 ** (-jnp.arange(0, DK, 2, dtype=F32) / DK)
        places = jnp.concatenate(
            [jnp.arange(BLOCK, dtype=jnp.int32), sp * rows + BLOCK * jnp.arange(blocks, dtype=jnp.int32)]
        )
        angles = places[:, None].astype(F32) * inverse[None, :]
        table = jnp.stack([jnp.cos(angles), jnp.sin(angles)])
        decay = log_decay.reshape(heads, blocks, BLOCK)
        halves = 2 // heads
        size = DK // halves
        table_spec = pl.BlockSpec(table.shape, lambda h: (0, 0, 0))
        decay_spec = pl.BlockSpec((1, blocks, BLOCK), lambda h: (h, 0, 0))
        key_spec = pl.BlockSpec((rows, DK), lambda h: (0, h))
        value_spec = pl.BlockSpec((rows, DV), lambda h: (0, h))
        y_word = y.astype(jnp.int32).reshape(1)
        payload = jax.ShapeDtypeStruct((size + TAIL, DV), BF)
        payload_spec = pl.BlockSpec(payload.shape, lambda h: (0, 0))
        word_spec = pl.BlockSpec(memory_space=pltpu.SMEM)
        mine, theirs = pl.pallas_call(
            functools.partial(state_kernel, halves=halves),
            out_shape=(payload, payload),
            grid=(heads,),
            in_specs=[word_spec, key_spec, value_spec, decay_spec, table_spec],
            out_specs=(payload_spec, payload_spec),
            scratch_shapes=[pltpu.VMEM((rows, DK), BF)],
            compiler_params=params(),
            name="state",
        )(y_word, keys, values, decay, table)

        local, query_decayed = pl.pallas_call(
            local_kernel,
            out_shape=(
                jax.ShapeDtypeStruct((rows, heads * DV), F32),
                jax.ShapeDtypeStruct((rows, heads * DK), BF),
            ),
            grid=(heads,),
            in_specs=[key_spec, key_spec, value_spec, decay_spec, table_spec],
            out_specs=(value_spec, key_spec),
            scratch_shapes=[pltpu.VMEM((DK, DV), F32)],
            compiler_params=params(),
            name="local",
        )(queries, keys, values, decay, table)

        def small(kernel, out_shape, *args):
            return pl.pallas_call(
                kernel,
                out_shape=out_shape,
                in_specs=[word_spec if arg is y_word else pl.BlockSpec(memory_space=pltpu.VMEM) for arg in args],
                compiler_params=params(),
            )(*args)

        got = swap_y(theirs)
        plane = upto = small(plane_kernel, payload, y_word, mine, got)
        sent = [forward_z(plane, 1)]
        reach = 2
        while reach < n_z:
            upto = small(upto_kernel, payload, plane, *sent)
            sent.append(forward_z(upto, reach))
            reach *= 2
        state_half = jax.ShapeDtypeStruct((size, DV), BF)
        send, keep = small(before_kernel, (state_half, state_half), y_word, mine, got, *sent)
        arrived_state = swap_y(send)

        def projected(order):
            count = order.shape[0]
            return pl.pallas_call(
                gate_kernel,
                out_shape=jax.ShapeDtypeStruct((count, own_rows, width), BF),
                grid_spec=pltpu.PrefetchScalarGridSpec(
                    num_scalar_prefetch=2,
                    grid=(count,),
                    in_specs=[
                        pl.BlockSpec((own_rows, heads * DV), lambda j, o, w: (o[j], 0)),
                        pl.BlockSpec((own_rows, heads * DK), lambda j, o, w: (o[j], 0)),
                        pl.BlockSpec((size, DV), lambda j, o, w: (0, 0)),
                        pl.BlockSpec((size, DV), lambda j, o, w: (0, 0)),
                        pl.BlockSpec((own_rows, heads * DV), lambda j, o, w: (o[j], 0)),
                        pl.BlockSpec(out_weight.shape, lambda j, o, w: (0, 0)),
                    ],
                    out_specs=pl.BlockSpec((1, own_rows, width), lambda j, o, w: (j, 0, 0)),
                    scratch_shapes=[pltpu.VMEM((own_rows, heads * DV), BF), pltpu.VMEM((2, size, DV), BF)],
                ),
                compiler_params=params(),
            )(order, y_word, local, query_decayed, keep, arrived_state, gates, out_weight)

        def places_of(steps):
            chips = [2 * ((x + s) % n_x) for s in steps]
            return jnp.stack([c + 1 - core for c in chips] + [c + core for c in chips]).astype(jnp.int32)

        far = projected(places_of(range(1, n_x)))
        near = projected(places_of([0]))
        far_sum = (swap_core(far[: n_x - 1]).astype(F32) + far[n_x - 1 :].astype(F32)).astype(BF)
        arrived = [shift_x(far_sum[s - 1], s) for s in range(1, n_x)]
        near_other = swap_core(near[0])

        steps = max(own_rows // 128, 1)
        tall = own_rows // steps
        row_spec = pl.BlockSpec((tall, width), lambda i, o: (i, 0))
        updated, normed = pl.pallas_call(
            functools.partial(norm_kernel, regions=n_sp),
            out_shape=(jax.ShapeDtypeStruct(resid.shape, BF), jax.ShapeDtypeStruct(resid.shape, BF)),
            grid_spec=pltpu.PrefetchScalarGridSpec(
                num_scalar_prefetch=1,
                grid=(steps,),
                in_specs=[row_spec] * (3 + n_x - 1) + [pl.BlockSpec((1, width), lambda i, o: (0, 0))],
                out_specs=(row_spec, row_spec),
            ),
            compiler_params=params(),
            name="norm",
        )(y_word, resid, near[1], near_other, *arrived, gain.reshape(1, width))

        z_word = z.astype(jnp.int32).reshape(1)

        def raised(sources):
            args = (z_word, *sources, *up)
            return pl.pallas_call(
                functools.partial(up_kernel, planes=n_z, sources=len(sources)),
                out_shape=jax.ShapeDtypeStruct((2 * own_rows, units), BF),
                in_specs=[pl.BlockSpec(memory_space=pltpu.SMEM)]
                + [pl.BlockSpec(memory_space=pltpu.VMEM)] * (len(args) - 1),
                out_specs=pl.BlockSpec(memory_space=pltpu.VMEM),
                compiler_params=params(),
                name="up",
            )(*args)

        def lowered(sources, side, kinds):
            args = (z_word, *sources, *down[side * n_z : (side + 1) * n_z])
            tall = len(sources) * own_rows
            mine, others = pl.pallas_call(
                functools.partial(down_kernel, planes=n_z),
                out_shape=(jax.ShapeDtypeStruct((tall, width // 2), BF),) * 2,
                in_specs=[pl.BlockSpec(memory_space=pltpu.SMEM)]
                + [pl.BlockSpec(memory_space=pltpu.VMEM)] * (len(args) - 1),
                out_specs=(pl.BlockSpec(memory_space=pltpu.VMEM),) * 2,
                compiler_params=params(),
                name="down",
            )(*args)
            others = swap_core(others)
            parts = [slice(i * own_rows, (i + 1) * own_rows) for i in range(len(sources))]
            sums = [
                (mine[part].astype(F32) + others[part].astype(F32)).astype(kind)
                for part, kind in zip(parts, kinds)
            ]
            return lax.optimization_barrier(tuple(sums))

        near_x = range(1, n_x)
        top = own_rows // 2
        upper, under = normed[:top], normed[top:]
        x_under = {s: shift_x(under, s) for s in near_x}
        z_upper = swap_z(upper)
        x_upper = {s: shift_x(upper, s) for s in near_x}
        z_under = swap_z(under)
        chunks = {"o": [normed], "z": [z_upper, z_under]}
        for s in near_x:
            chunks[f"x{s}"] = [x_upper[s], x_under[s]]
            chunks[f"c{s}"] = [shift_x(z_upper, s), swap_z(x_under[s])]
        hidden = {key: raised(parts + [swap_core(part) for part in parts]) for key, parts in chunks.items()}
        straight = [hidden[f"x{s}"] for s in near_x] + [hidden["z"], hidden["o"]]
        corners = [hidden[f"c{s}"] for s in near_x]

        def home(value, s):
            return shift_x(value.astype(BF), n_x - s).astype(F32)

        (left_z,) = lowered([hidden["z"]], 0, [F32])
        *left_x, left_sum = lowered(straight[:-2] + straight[-1:], 0, [BF] * (n_x - 1) + [F32])
        left_c = lowered(corners, 0, [BF] * (n_x - 1))
        (right_z,) = lowered([hidden["z"]], 1, [BF])
        *right_x, right_sum = lowered(straight[:-2] + straight[-1:], 1, [F32] * n_x)
        right_c = lowered(corners, 1, [BF] * (n_x - 1))
        for s in near_x:
            left_sum = left_sum + home(left_x[s - 1], s)
            left_z = left_z + home(left_c[s - 1], s)
        right_sum = right_sum + swap_z(right_z.astype(BF)).astype(F32)
        right_x = [right_x[s - 1] + swap_z(right_c[s - 1].astype(BF)).astype(F32) for s in near_x]
        left_sum = left_sum + swap_z(left_z.astype(BF)).astype(F32)
        for s in near_x:
            right_sum = right_sum + home(right_x[s - 1], s)
        pieces = [left_sum, right_sum]

        return pl.pallas_call(
            functools.partial(last_kernel, regions=n_sp),
            out_shape=jax.ShapeDtypeStruct(resid.shape, BF),
            grid_spec=pltpu.PrefetchScalarGridSpec(
                num_scalar_prefetch=1,
                grid=(steps,),
                in_specs=[row_spec] + [pl.BlockSpec((tall, width // 2), lambda i, o: (i, 0))] * 2,
                out_specs=row_spec,
            ),
            compiler_params=params(),
            name="last",
        )(y_word, updated, *pieces)

    return body


def solution(mesh):
    placed = (
        P(("sp", "tp"), None),
        P("sp", "tp"),
        P("sp", "tp"),
        P("sp", "tp"),
        P("sp", "tp"),
        P("tp", "sp"),
        P("tp", None),
        P(),
        P("sp", "tp"),
        P("tp", "sp"),
    )
    n_sp, n_tp = mesh.shape["sp"], mesh.shape["tp"]
    body = make_body(n_sp, n_tp)

    return jax.shard_map(body, mesh=mesh, in_specs=placed, out_specs=P(("sp", "tp"), None), check_vma=False)
```
